32 devices in a mesh: grp: 2 (over y), sp: 4 (over z), tp: 4 (over x, core).
Axes of the slice: x: 2, y: 2, z: 4, core: 2. Of those that a mesh axis runs over, the one named last changes fastest.
Arguments:
- tokens: bfloat16 [24576, 2048], P(('grp', 'sp', 'tp')), parts along dimension 0, may hold values from -6 to 6
- gain_pre: float32 [2, 2048], replicated, may hold values from 0.1 to 1.9
- gain_post: float32 [2, 2048], replicated, may hold values from 0.1 to 1.9
- w_b: bfloat16 [2, 2048, 512], P(None, 'sp', 'tp'), may hold values from -0.125 to 0.125
- w_c: bfloat16 [2, 2048, 512], P(None, 'sp', 'tp'), may hold values from -0.125 to 0.125
- w_x: bfloat16 [2, 2048, 512], P(None, 'sp', 'tp'), may hold values from -0.125 to 0.125
- taps: float32 [2, 3, 512], replicated, may hold values from -3.5 to 3.5
- w_out: bfloat16 [2, 512, 2048], P(None, 'tp', 'sp'), may hold values from -0.25 to 0.25
Outputs:
- result: bfloat16 [24576, 2048], P(('grp', 'sp', 'tp')), parts along dimension 0
The draws below stay inside these ranges and needn't reach their ends.
There are 2 independent parts, one for each index of `grp`. The reference program is written for one: setup_inputs(seed, part) draws one part's arguments, and reference() takes and returns one part's arrays. A program takes and returns all parts, laid end to end along the dimension named above; an argument that names none is the same for every part. Nothing has to cross between parts.
All inputs are finite; a program needn't handle non-finite values.
Results may differ from the reference program's by a relative error of at most 0.024.
Values may be sent and summed in bfloat16 or wider, within the bound.
A program may use at most 128 MiB of HBM per device.

```python
import jax
import jax.numpy as jnp
from jax import lax

D = 2048
DC = 512
KERNEL = 3
LAYERS = 2
TOKENS = 12288


def level_of(own_key, dims, cuts, least, high):
    def one(dim, parts):
        draws = jax.random.uniform(jax.random.fold_in(jax.random.fold_in(own_key, 6), dim), (parts,), jnp.float32, least / len(cuts), high / len(cuts))
        return jnp.repeat(jnp.exp(draws), dims[dim] // parts).reshape((-1,) + (1,) * (len(dims) - dim - 1))

    gain = one(*cuts[0])
    for cut in cuts[1:]:
        gain = gain * one(*cut)
    return gain


def centred(stream_key, extent, scale, reach, cuts=(), held_as=jnp.bfloat16):
    result = jax.random.normal(stream_key, extent, jnp.float32) * scale
    if len(cuts) > 0:
        result = level_of(stream_key, extent, cuts, -0.22, 0.18) * result
    return jnp.clip(result, min=-reach, max=reach).astype(held_as)


def setup_inputs(seed: int = 0, part: int = 0) -> dict:
    key_of = jax.random.split(jax.random.key(seed), 9)
    part_splits = jax.random.split(jax.random.fold_in(key_of[8], part), 9)
    return {
        "tokens": centred(part_splits[0], (TOKENS, D), 1.0, 6.0, ((0, 16),)),
        "gain_pre": jnp.clip(1.0 + 0.18 * jax.random.normal(key_of[1], (LAYERS, D), jnp.float32), 0.1, 1.9),
        "gain_post": jnp.clip(1.0 + 0.18 * jax.random.normal(key_of[2], (LAYERS, D), jnp.float32), 0.1, 1.9),
        "w_b": centred(key_of[3], (LAYERS, D, DC), D ** -0.5, 0.125, ((1, 4), (2, 4))),
        "w_c": centred(key_of[4], (LAYERS, D, DC), D ** -0.5, 0.125, ((1, 4), (2, 4))),
        "w_x": centred(key_of[5], (LAYERS, D, DC), D ** -0.5, 0.125, ((1, 4), (2, 4))),
        "taps": centred(key_of[6], (LAYERS, KERNEL, DC), KERNEL ** -0.5, 3.5, (), jnp.float32),
        "w_out": centred(key_of[7], (LAYERS, DC, D), DC ** -0.5, 0.25, ((1, 4), (2, 4))),
    }


epsilon = 1e-06

def normed(activations, gain_row):
    values_f = activations.astype(jnp.float32)
    scale = lax.rsqrt(lax.optimization_barrier(jnp.mean(values_f * values_f, axis=-1, keepdims=True)) + epsilon)
    return values_f * scale * gain_row

def reference(tokens, gain_pre, gain_post, w_b, w_c, w_x, taps, w_out):
    stream = tokens
    for layer_index in range(LAYERS):
        hidden = normed(stream, gain_pre[layer_index]).astype(jnp.bfloat16)
        gate_b = jnp.dot(hidden, w_b[layer_index], preferred_element_type=jnp.float32).astype(jnp.bfloat16)
        gate_c = jnp.dot(hidden, w_c[layer_index], preferred_element_type=jnp.float32).astype(jnp.bfloat16)
        values = jnp.dot(hidden, w_x[layer_index], preferred_element_type=jnp.float32).astype(jnp.bfloat16)
        product = (gate_c.astype(jnp.float32) * values.astype(jnp.float32)).astype(jnp.bfloat16)
        padded = jnp.pad(product.astype(jnp.float32), ((KERNEL - 1, 0), (0, 0)))
        row_total = padded.shape[0] - KERNEL + 1
        convolved = jnp.zeros((row_total, DC), jnp.float32)
        for offset in range(KERNEL):
            convolved = convolved + taps[layer_index, offset][None, :] * padded[offset:offset + row_total]
        weighted = (gate_b.astype(jnp.float32) * convolved).astype(jnp.bfloat16)
        branch = jnp.dot(weighted, w_out[layer_index], preferred_element_type=jnp.float32)
        stream = (stream.astype(jnp.float32) + normed(branch, gain_post[layer_index])).astype(jnp.bfloat16)
    return stream
```

```python
import functools

import jax
import jax.numpy as jnp
from jax import lax
from jax.experimental import pallas as pl
from jax.experimental.pallas import tpu as pltpu
from jax.sharding import PartitionSpec as P

epsilon = 1e-06
MESH = pl.DeviceIdType.MESH


def for_sending(value):
    return jax.tree.map(lambda a: a.astype(jnp.bfloat16) if a.dtype == jnp.float32 else a, value)


def from_behind(block, axis, distance):
    devices = range(lax.axis_size(axis))
    route = [(i - distance, i) for i in devices if i - distance in devices]
    return lax.ppermute(block, axis, route)


def normed(activations, gain_row):
    values_f = activations.astype(jnp.float32)
    scale = lax.rsqrt(jnp.mean(values_f * values_f, axis=-1, keepdims=True) + epsilon)
    return values_f * scale * gain_row


def fold_into(hidden, pieces):
    return tuple(
        (
            jnp.dot(hidden, weight_piece, preferred_element_type=jnp.float32)
            for weight_piece in pieces
        )
    )


def convolve(extended, tap_rows):
    kernel_size = tap_rows.shape[0]
    row_total = extended.shape[0] - kernel_size + 1
    extended_f = extended.astype(jnp.float32)
    convolved = jnp.zeros((row_total, extended.shape[1]), jnp.float32)
    for offset in range(kernel_size):
        convolved = convolved + tap_rows[offset][None, :] * extended_f[offset : offset + row_total]
    return convolved


def layer_blocks(w_b, w_c, w_x, w_out, layer_index):
    return (
        lax.all_gather(w_b[layer_index], "tp", axis=1, tiled=True),
        lax.all_gather(w_c[layer_index], "tp", axis=1, tiled=True),
        lax.all_gather(w_x[layer_index], "tp", axis=1, tiled=True),
        lax.all_gather(w_out[layer_index], "tp", axis=0, tiled=True),
    )


def gated_inputs(stream, gain_row, weights):
    hidden = normed(stream, gain_row).astype(jnp.bfloat16)
    sums = fold_into(
        hidden,
        jax.tree.map(
            lambda part: lax.all_gather(part, "sp", axis=0, tiled=True), for_sending(weights)
        ),
    )
    gate_b, gate_c, values = (item.astype(jnp.bfloat16) for item in sums)
    product = (gate_c.astype(jnp.float32) * values.astype(jnp.float32)).astype(jnp.bfloat16)
    return (gate_b, product)


def mixed_output(residual, gate_b, extended, tap_rows, out_weight, gain_row):
    convolved = convolve(extended, tap_rows)
    weighted = (gate_b.astype(jnp.float32) * convolved).astype(jnp.bfloat16)
    branch = jnp.dot(
        weighted,
        lax.all_gather(out_weight, "sp", axis=1, tiled=True),
        preferred_element_type=jnp.float32,
    )
    return (residual.astype(jnp.float32) + normed(branch, gain_row)).astype(jnp.bfloat16)


def on_device(tokens, gain_pre, gain_post, w_b, w_c, w_x, taps, w_out):
    layer_total = gain_pre.shape[0]
    kernel_size = taps.shape[1]
    reach = kernel_size - 1
    stream = tokens
    before = from_behind(stream[-reach * layer_total :], ("sp", "tp"), 1)
    stream = jnp.concatenate([before, stream], axis=0)
    for layer_index in range(layer_total):
        blocks = layer_blocks(w_b, w_c, w_x, w_out, layer_index)
        gate_b, product = gated_inputs(stream, gain_pre[layer_index], blocks[:3])
        stream = mixed_output(
            stream[reach:],
            gate_b[reach:],
            product,
            taps[layer_index],
            blocks[3],
            gain_post[layer_index],
        )
    return stream


def unit_views(units, win, wout):
    def view(unit, s, t, start, count, rows, cols):
        layer, kind = units[unit]
        if kind == 0:
            return win.at[
                layer,
                :,
                pl.ds(pl.multiple_of(s * rows + start, 16), count),
                pl.ds(pl.multiple_of(t * cols, 128), cols),
            ]
        return wout.at[
            layer,
            pl.ds(pl.multiple_of(t * cols + start, 16), count),
            pl.ds(pl.multiple_of(s * rows, 128), rows),
        ]

    return view


def up_to(fraction_num, fraction_den, total):
    return -(-(total * fraction_num // fraction_den) // 16) * 16


def mixer_kernel(
    sp, tp, halo, tok, gain_pre, gain_post, w_b, w_c, w_x, taps, w_out, out,
    win, wout, xs, hid, gated, prod,
    load_sem, halo_sem, z_send, z_recv, x_send, x_recv, y1_send, y1_recv,
    y2_send, y2_recv, d_send, d_recv, out_sem,
):
    layers = w_b.shape[0]
    rows, cols = w_b.shape[1], w_b.shape[2]
    own_tokens = tok.shape[0]
    total_rows = own_tokens + halo
    channels = win.shape[3]
    y = lax.axis_index("grp")
    z = lax.axis_index("sp")
    t = lax.axis_index("tp")
    core = lax.rem(t, 2)
    x = t // 2
    t_x = (1 - x) * 2 + core
    t_core = x * 2 + 1 - core
    t_both = (1 - x) * 2 + 1 - core
    units = [(layer, kind) for layer in range(layers) for kind in (0, 1)]
    view = unit_views(units, win, wout)

    def sizes(unit):
        n = rows if units[unit][1] == 0 else cols
        return n, up_to(3, 4, n), up_to(19, 32, n)

    def block(unit, s, tt, start, count):
        return view(unit, s, tt, start, count, rows, cols)

    def send(ref, send_sem, recv_sem, where):
        return pltpu.make_async_remote_copy(
            src_ref=ref, dst_ref=ref, send_sem=send_sem, recv_sem=recv_sem,
            device_id=where, device_id_type=MESH,
        )

    def z_copy(u, s, up):
        n, nz, _ = sizes(u)
        return send(
            block(u, s, t, y * (n - nz), nz), z_send.at[u, s, up], z_recv.at[u, s],
            {"sp": z + (1 if up else -1)},
        )

    def x_copy(u, s, tt):
        n, _, nx = sizes(u)
        return send(
            block(u, s, tt, y * (n - nx), nx), x_send.at[u, s], x_recv.at[u, s], {"tp": t_x}
        )

    def y1_copy(u, s, yy):
        n, nz, _ = sizes(u)
        return send(
            block(u, s, t, yy * nz, n - nz), y1_send.at[u, s], y1_recv.at[u, s], {"grp": 1 - y}
        )

    def y2_copy(u, s, yy):
        n, _, nx = sizes(u)
        return send(
            block(u, s, t_x, yy * nx, n - nx), y2_send.at[u, s], y2_recv.at[u, s], {"grp": 1 - y}
        )

    def d_copy(u, s, other, tt):
        n, _, _ = sizes(u)
        return send(
            block(u, s, tt, 0, n), d_send.at[u, s, other], d_recv.at[u, s, other], {"tp": t_core}
        )

    def at_distance(j, act):
        if j == 0:
            act(z, None)
            return

        @pl.when(z + j < sp)
        def _():
            act(z + j, 0)

        @pl.when(z >= j)
        def _():
            act(z - j, 1)

    def own(u):
        @pl.when(z + 1 < sp)
        def _():
            z_copy(u, z, 1).start()

        @pl.when(z >= 1)
        def _():
            z_copy(u, z, 0).start()

        x_copy(u, z, t).start()
        d_copy(u, z, 0, t).start()

    def wave_z(u, j):
        def act(s, up):
            z_copy(u, s, up).wait_recv()
            if up:
                @pl.when(z + 1 < sp)
                def _():
                    z_copy(u, s, 1).start()
            else:
                @pl.when(z >= 1)
                def _():
                    z_copy(u, s, 0).start()
            x_copy(u, s, t).start()
            y1_copy(u, s, y).start()

        at_distance(j, act)

    def wave_x(u, j):
        def act(s, _):
            x_copy(u, s, t_x).wait_recv()
            y2_copy(u, s, y).start()

        at_distance(j, act)

    def wave_y(u, j):
        def act(s, _):
            if j > 0:
                y1_copy(u, s, 1 - y).wait_recv()
                d_copy(u, s, 0, t).start()
            y2_copy(u, s, 1 - y).wait_recv()
            d_copy(u, s, 1, t_x).start()

        at_distance(j, act)

    def arrived(u):
        for j in range(sp):
            def act(s, _):
                d_copy(u, s, 0, t_core).wait_recv()
                d_copy(u, s, 1, t_both).wait_recv()

            at_distance(j, act)

    def sent(u):
        for j in range(sp):
            def act(s, up):
                if j == 0:
                    @pl.when(z + 1 < sp)
                    def _():
                        z_copy(u, s, 1).wait_send()

                    @pl.when(z >= 1)
                    def _():
                        z_copy(u, s, 0).wait_send()
                else:
                    if up:
                        @pl.when(z + 1 < sp)
                        def _():
                            z_copy(u, s, 1).wait_send()
                    else:
                        @pl.when(z >= 1)
                        def _():
                            z_copy(u, s, 0).wait_send()
                    y1_copy(u, s, y).wait_send()
                x_copy(u, s, t).wait_send()
                y2_copy(u, s, y).wait_send()
                d_copy(u, s, 0, t).wait_send()
                d_copy(u, s, 1, t_x).wait_send()

            at_distance(j, act)

    def scaled(value_f, gain_row):
        scale = lax.rsqrt(jnp.mean(value_f * value_f, axis=-1, keepdims=True) + epsilon)
        return value_f * scale * gain_row

    def project_in(layer, part, width):
        cut = pl.ds(part * width, width)
        hidden = hid[...]

        def through(which):
            return jnp.dot(
                hidden, win[layer, which, :, cut], preferred_element_type=jnp.float32
            ).astype(jnp.bfloat16).astype(jnp.float32)

        product = (through(1) * through(2)).astype(jnp.bfloat16).astype(jnp.float32)
        reach = taps.shape[1] - 1
        prod[pl.ds(8, total_rows), :] = product
        conv = taps[layer, reach, cut][None, :] * product
        for k in range(reach):
            conv = conv + taps[layer, k, cut][None, :] * prod[pl.ds(8 - reach + k, total_rows), :]
        gated[:, cut] = (through(0) * conv).astype(jnp.bfloat16)

    def project_out(layer, start, count):
        where = pl.ds(start, count)
        branch = jnp.dot(gated[where, :], wout[layer], preferred_element_type=jnp.float32)
        added = xs[where, :].astype(jnp.float32) + scaled(branch, gain_post[layer][None, :])
        stream = added.astype(jnp.bfloat16)
        xs[where, :] = stream
        if layer + 1 < layers:
            hid[where, :] = scaled(
                stream.astype(jnp.float32), gain_pre[layer + 1][None, :]
            ).astype(jnp.bfloat16)

    loads = []
    for layer in range(layers):
        for which, ref in enumerate((w_b, w_c, w_x)):
            loads.append(
                pltpu.make_async_copy(
                    ref.at[layer],
                    win.at[
                        layer,
                        which,
                        pl.ds(pl.multiple_of(z * rows, 16), rows),
                        pl.ds(pl.multiple_of(t * cols, 128), cols),
                    ],
                    load_sem.at[4 * layer + which],
                )
            )
        loads.append(
            pltpu.make_async_copy(
                w_out.at[layer],
                wout.at[
                    layer,
                    pl.ds(pl.multiple_of(t * cols, 16), cols),
                    pl.ds(pl.multiple_of(z * rows, 128), rows),
                ],
                load_sem.at[4 * layer + 3],
            )
        )
    tokens_in = pltpu.make_async_copy(
        tok, xs.at[pl.ds(halo, own_tokens)], load_sem.at[4 * layers]
    )
    for load in loads:
        load.start()
    tokens_in.start()

    place = z * tp + t
    after = lax.rem(place + 1, sp * tp)

    def halo_copy():
        return pltpu.make_async_remote_copy(
            src_ref=tok.at[pl.ds(own_tokens - halo, halo)],
            dst_ref=xs.at[pl.ds(0, halo)],
            send_sem=halo_sem.at[0],
            recv_sem=halo_sem.at[1],
            device_id={"sp": after // tp, "tp": lax.rem(after, tp)},
            device_id_type=MESH,
        )

    for load in loads:
        load.wait()
    own(0)

    @pl.when(place + 1 < sp * tp)
    def _():
        halo_copy().start()

    own(1)
    prod[pl.ds(0, 8), :] = jnp.zeros((8, prod.shape[1]), jnp.float32)

    @pl.when(place == 0)
    def _():
        xs[pl.ds(0, halo), :] = jnp.zeros((halo, xs.shape[1]), jnp.bfloat16)

    tokens_in.wait()

    def first_norm(start, count):
        where = pl.ds(start, count)
        hid[where, :] = scaled(xs[where, :].astype(jnp.float32), gain_pre[0][None, :]).astype(
            jnp.bfloat16
        )

    piece = own_tokens // 3
    for i in range(3):
        first_norm(halo + i * piece, piece)

    @pl.when(place > 0)
    def _():
        halo_copy().wait_recv()

    first_norm(0, halo)

    steps = sp - 1
    width = prod.shape[1]
    parts = channels // width
    work = {}

    def result_copy(i):
        return pltpu.make_async_copy(
            xs.at[pl.ds(halo + i * piece, piece)],
            out.at[pl.ds(i * piece, piece)],
            out_sem.at[i],
        )

    def last_rows(layer, i):
        project_out(layer, halo + i * piece, piece)
        if layer == layers - 1:
            result_copy(i).start()

    last_step = steps * len(units) + 2
    for u, (layer, kind) in enumerate(units):
        ready = min(steps * u + steps + 2, last_step)
        todo = [functools.partial(arrived, u)]
        if kind == 0:
            todo += [functools.partial(project_in, layer, p, width) for p in range(parts)]
        else:
            todo += [functools.partial(last_rows, layer, i) for i in range(3)]
            if layer + 1 < layers:
                todo.append(functools.partial(project_out, layer, 0, halo))
        for k, task in enumerate(todo):
            work.setdefault(min(ready + max(k - 1, 0), last_step), []).append(task)

    for g in range(1, last_step + 1):
        u, j = (g - 1) // steps, (g - 1) % steps + 1
        if u < len(units):
            if j == 1 and 1 <= u < len(units) - 1:
                own(u + 1)
            wave_z(u, j)
        for late, wave in ((1, wave_x), (2, wave_y)):
            v, k = (g - 1 - late) // steps, (g - 1 - late) % steps + 1
            if k == 1 and 0 <= v < len(units):
                wave(v, 0)
            if 0 <= v < len(units):
                wave(v, k)
        for task in work.get(g, []):
            task()

    for u in range(len(units)):
        sent(u)

    @pl.when(place + 1 < sp * tp)
    def _():
        halo_copy().wait_send()

    for i in range(3):
        result_copy(i).wait()


def in_one_kernel(sp, tp, tokens, gain_pre, gain_post, w_b, w_c, w_x, taps, w_out):
    layers, rows, cols = w_b.shape
    own_tokens, width = tokens.shape
    channels = cols * tp
    halo = 16
    units = 2 * layers
    any_space = pl.BlockSpec(memory_space=pl.ANY)
    vmem = pl.BlockSpec(memory_space=pltpu.VMEM)
    dma = pltpu.SemaphoreType.DMA
    part = min(256, channels)
    return pl.pallas_call(
        functools.partial(mixer_kernel, sp, tp, halo),
        out_shape=jax.ShapeDtypeStruct(tokens.shape, tokens.dtype),
        in_specs=[any_space, vmem, vmem, any_space, any_space, any_space, vmem, any_space],
        out_specs=any_space,
        scratch_shapes=[
            pltpu.VMEM((layers, 3, rows * sp, channels), jnp.bfloat16),
            pltpu.VMEM((layers, channels, rows * sp), jnp.bfloat16),
            pltpu.VMEM((own_tokens + halo, width), jnp.bfloat16),
            pltpu.VMEM((own_tokens + halo, width), jnp.bfloat16),
            pltpu.VMEM((own_tokens + halo, channels), jnp.bfloat16),
            pltpu.VMEM((own_tokens + halo + 8, part), jnp.float32),
            dma((4 * layers + 1,)),
            dma((2,)),
            dma((units, sp, 2)),
            dma((units, sp)),
            dma((units, sp)),
            dma((units, sp)),
            dma((units, sp)),
            dma((units, sp)),
            dma((units, sp)),
            dma((units, sp)),
            dma((units, sp, 2)),
            dma((units, sp, 2)),
            dma((3,)),
        ],
        compiler_params=pltpu.CompilerParams(
            has_side_effects=True, vmem_limit_bytes=60 * 1024 * 1024
        ),
    )(tokens, gain_pre, gain_post, w_b, w_c, w_x, taps, w_out)


def kernel_fits(sizes, tokens, w_b, w_out, taps):
    rows, cols = w_b.shape[1], w_b.shape[2]
    layers = w_b.shape[0]
    held = (4 * layers * rows * sizes["sp"] * cols * sizes["tp"]) * 2
    held += 3 * tokens.shape[0] * tokens.shape[1] * 2
    return (
        sizes["grp"] == 2
        and sizes["tp"] == 4
        and rows % 128 == 0
        and cols % 128 == 0
        and tokens.shape[0] % 48 == 0
        and (taps.shape[1] - 1) * layers <= 16
        and taps.shape[1] <= 9
        and held < 40 * 2**20
    )


def any_mesh(sizes, *arguments):
    tokens, w_b, taps, w_out = arguments[0], arguments[3], arguments[6], arguments[7]
    if kernel_fits(sizes, tokens, w_b, w_out, taps):
        return in_one_kernel(sizes["sp"], sizes["tp"], *arguments)
    return on_device(*arguments)


def solution(mesh):
    placed = (
        P(("grp", "sp", "tp"), None),
        P(),
        P(),
        P(None, "sp", "tp"),
        P(None, "sp", "tp"),
        P(None, "sp", "tp"),
        P(),
        P(None, "tp", "sp"),
    )
    return jax.shard_map(
        functools.partial(any_mesh, dict(mesh.shape)),
        mesh=mesh,
        in_specs=placed,
        out_specs=P(("grp", "sp", "tp"), None),
        check_vma=False,
    )
```

```python
import functools

import jax
import jax.numpy as jnp
from jax import lax
from jax.experimental import pallas as pl
from jax.experimental.pallas import tpu as pltpu
from jax.sharding import PartitionSpec as P

epsilon = 1e-06
MESH = pl.DeviceIdType.MESH


def for_sending(value):
    return jax.tree.map(lambda a: a.astype(jnp.bfloat16) if a.dtype == jnp.float32 else a, value)


def from_behind(block, axis, distance):
    devices = range(lax.axis_size(axis))
    route = [(i - distance, i) for i in devices if i - distance in devices]
    return lax.ppermute(block, axis, route)


def normed(activations, gain_row):
    values_f = activations.astype(jnp.float32)
    scale = lax.rsqrt(jnp.mean(values_f * values_f, axis=-1, keepdims=True) + epsilon)
    return values_f * scale * gain_row


def fold_into(hidden, pieces):
    return tuple(
        (
            jnp.dot(hidden, weight_piece, preferred_element_type=jnp.float32)
            for weight_piece in pieces
        )
    )


def convolve(extended, tap_rows):
    kernel_size = tap_rows.shape[0]
    row_total = extended.shape[0] - kernel_size + 1
    extended_f = extended.astype(jnp.float32)
    convolved = jnp.zeros((row_total, extended.shape[1]), jnp.float32)
    for offset in range(kernel_size):
        convolved = convolved + tap_rows[offset][None, :] * extended_f[offset : offset + row_total]
    return convolved


def layer_blocks(w_b, w_c, w_x, w_out, layer_index):
    return (
        lax.all_gather(w_b[layer_index], "tp", axis=1, tiled=True),
        lax.all_gather(w_c[layer_index], "tp", axis=1, tiled=True),
        lax.all_gather(w_x[layer_index], "tp", axis=1, tiled=True),
        lax.all_gather(w_out[layer_index], "tp", axis=0, tiled=True),
    )


def gated_inputs(stream, gain_row, weights):
    hidden = normed(stream, gain_row).astype(jnp.bfloat16)
    sums = fold_into(
        hidden,
        jax.tree.map(
            lambda part: lax.all_gather(part, "sp", axis=0, tiled=True), for_sending(weights)
        ),
    )
    gate_b, gate_c, values = (item.astype(jnp.bfloat16) for item in sums)
    product = (gate_c.astype(jnp.float32) * values.astype(jnp.float32)).astype(jnp.bfloat16)
    return (gate_b, product)


def mixed_output(residual, gate_b, extended, tap_rows, out_weight, gain_row):
    convolved = convolve(extended, tap_rows)
    weighted = (gate_b.astype(jnp.float32) * convolved).astype(jnp.bfloat16)
    branch = jnp.dot(
        weighted,
        lax.all_gather(out_weight, "sp", axis=1, tiled=True),
        preferred_element_type=jnp.float32,
    )
    return (residual.astype(jnp.float32) + normed(branch, gain_row)).astype(jnp.bfloat16)


def on_device(tokens, gain_pre, gain_post, w_b, w_c, w_x, taps, w_out):
    layer_total = gain_pre.shape[0]
    kernel_size = taps.shape[1]
    reach = kernel_size - 1
    stream = tokens
    before = from_behind(stream[-reach * layer_total :], ("sp", "tp"), 1)
    stream = jnp.concatenate([before, stream], axis=0)
    for layer_index in range(layer_total):
        blocks = layer_blocks(w_b, w_c, w_x, w_out, layer_index)
        gate_b, product = gated_inputs(stream, gain_pre[layer_index], blocks[:3])
        stream = mixed_output(
            stream[reach:],
            gate_b[reach:],
            product,
            taps[layer_index],
            blocks[3],
            gain_post[layer_index],
        )
    return stream


def unit_views(units, win, wout):
    def view(unit, s, t, start, count, rows, cols):
        layer, kind = units[unit]
        if kind < 3:
            return win.at[
                layer,
                kind,
                pl.ds(pl.multiple_of(s * rows + start, 16), count),
                pl.ds(pl.multiple_of(t * cols, 128), cols),
            ]
        return wout.at[
            layer,
            pl.ds(pl.multiple_of(t * cols + start, 16), count),
            pl.ds(pl.multiple_of(s * rows, 128), rows),
        ]

    return view


def up_to(fraction_num, fraction_den, total):
    return -(-(total * fraction_num // fraction_den) // 16) * 16


def mixer_kernel(
    sp, tp, halo, tok, gain_pre, gain_post, w_b, w_c, w_x, taps, w_out, out,
    win, wout, xs, hid, gated, prod,
    load_sem, halo_sem, z_send, z_recv, x_send, x_recv, y1_send, y1_recv,
    y2_send, y2_recv, d_send, d_recv,
):
    layers = w_b.shape[0]
    rows, cols = w_b.shape[1], w_b.shape[2]
    own_tokens = tok.shape[0]
    total_rows = own_tokens + halo
    channels = win.shape[3]
    y = lax.axis_index("grp")
    z = lax.axis_index("sp")
    t = lax.axis_index("tp")
    core = lax.rem(t, 2)
    x = t // 2
    t_x = (1 - x) * 2 + core
    t_core = x * 2 + 1 - core
    t_both = (1 - x) * 2 + 1 - core
    units = [(layer, kind) for layer in range(layers) for kind in range(4)]
    view = unit_views(units, win, wout)

    def sizes(unit):
        n = rows if units[unit][1] < 3 else cols
        return n, up_to(3, 4, n), up_to(19, 32, n)

    def block(unit, s, tt, start, count):
        return view(unit, s, tt, start, count, rows, cols)

    def send(ref, send_sem, recv_sem, where):
        return pltpu.make_async_remote_copy(
            src_ref=ref, dst_ref=ref, send_sem=send_sem, recv_sem=recv_sem,
            device_id=where, device_id_type=MESH,
        )

    def z_copy(u, s, up):
        n, nz, _ = sizes(u)
        return send(
            block(u, s, t, y * (n - nz), nz), z_send.at[u, s, up], z_recv.at[u, s],
            {"sp": z + (1 if up else -1)},
        )

    def x_copy(u, s, tt):
        n, _, nx = sizes(u)
        return send(
            block(u, s, tt, y * (n - nx), nx), x_send.at[u, s], x_recv.at[u, s], {"tp": t_x}
        )

    def y1_copy(u, s, yy):
        n, nz, _ = sizes(u)
        return send(
            block(u, s, t, yy * nz, n - nz), y1_send.at[u, s], y1_recv.at[u, s], {"grp": 1 - y}
        )

    def y2_copy(u, s, yy):
        n, _, nx = sizes(u)
        return send(
            block(u, s, t_x, yy * nx, n - nx), y2_send.at[u, s], y2_recv.at[u, s], {"grp": 1 - y}
        )

    def d_copy(u, s, other, tt):
        n, _, _ = sizes(u)
        return send(
            block(u, s, tt, 0, n), d_send.at[u, s, other], d_recv.at[u, s, other], {"tp": t_core}
        )

    def at_distance(j, act):
        if j == 0:
            act(z, None)
            return

        @pl.when(z + j < sp)
        def _():
            act(z + j, 0)

        @pl.when(z >= j)
        def _():
            act(z - j, 1)

    def own(u):
        @pl.when(z + 1 < sp)
        def _():
            z_copy(u, z, 1).start()

        @pl.when(z >= 1)
        def _():
            z_copy(u, z, 0).start()

        x_copy(u, z, t).start()
        d_copy(u, z, 0, t).start()

    def wave_z(u, j):
        def act(s, up):
            z_copy(u, s, up).wait_recv()
            if up:
                @pl.when(z + 1 < sp)
                def _():
                    z_copy(u, s, 1).start()
            else:
                @pl.when(z >= 1)
                def _():
                    z_copy(u, s, 0).start()
            x_copy(u, s, t).start()
            y1_copy(u, s, y).start()

        at_distance(j, act)

    def wave_x(u, j):
        def act(s, _):
            x_copy(u, s, t_x).wait_recv()
            y2_copy(u, s, y).start()

        at_distance(j, act)

    def wave_y(u, j):
        def act(s, _):
            if j > 0:
                y1_copy(u, s, 1 - y).wait_recv()
                d_copy(u, s, 0, t).start()
            y2_copy(u, s, 1 - y).wait_recv()
            d_copy(u, s, 1, t_x).start()

        at_distance(j, act)

    def arrived(u):
        for j in range(sp):
            def act(s, _):
                d_copy(u, s, 0, t_core).wait_recv()
                d_copy(u, s, 1, t_both).wait_recv()

            at_distance(j, act)

    def sent(u):
        for j in range(sp):
            def act(s, up):
                if j == 0:
                    @pl.when(z + 1 < sp)
                    def _():
                        z_copy(u, s, 1).wait_send()

                    @pl.when(z >= 1)
                    def _():
                        z_copy(u, s, 0).wait_send()
                else:
                    if up:
                        @pl.when(z + 1 < sp)
                        def _():
                            z_copy(u, s, 1).wait_send()
                    else:
                        @pl.when(z >= 1)
                        def _():
                            z_copy(u, s, 0).wait_send()
                    y1_copy(u, s, y).wait_send()
                x_copy(u, s, t).wait_send()
                y2_copy(u, s, y).wait_send()
                d_copy(u, s, 0, t).wait_send()
                d_copy(u, s, 1, t_x).wait_send()

            at_distance(j, act)

    def scaled(value_f, gain_row):
        scale = lax.rsqrt(jnp.mean(value_f * value_f, axis=-1, keepdims=True) + epsilon)
        return value_f * scale * gain_row

    def project_in(layer, part, width):
        cut = pl.ds(part * width, width)
        hidden = hid[...]

        def through(which):
            return jnp.dot(
                hidden, win[layer, which, :, cut], preferred_element_type=jnp.float32
            ).astype(jnp.bfloat16).astype(jnp.float32)

        product = (through(1) * through(2)).astype(jnp.bfloat16).astype(jnp.float32)
        reach = taps.shape[0] - 1
        prod[pl.ds(8, total_rows), :] = product
        conv = taps[reach, layer, cut][None, :] * product
        for k in range(reach):
            conv = conv + taps[k, layer, cut][None, :] * prod[pl.ds(8 - reach + k, total_rows), :]
        gated[:, cut] = (through(0) * conv).astype(jnp.bfloat16)

    def project_out(layer, start, count):
        where = pl.ds(start, count)
        branch = jnp.dot(gated[where, :], wout[layer], preferred_element_type=jnp.float32)
        added = xs[where, :].astype(jnp.float32) + scaled(branch, gain_post[layer][None, :])
        stream = added.astype(jnp.bfloat16)
        if layer + 1 < layers:
            xs[where, :] = stream
            hid[where, :] = scaled(
                stream.astype(jnp.float32), gain_pre[layer + 1][None, :]
            ).astype(jnp.bfloat16)
        else:
            out[pl.ds(start - halo, count), :] = stream

    place = z * tp + t
    ready = pltpu.get_barrier_semaphore()

    def greet(where):
        pl.semaphore_signal(ready, inc=1, device_id=where, device_id_type=MESH)

    for where in ({"tp": t_x}, {"tp": t_core}, {"grp": 1 - y}):
        greet(where)

    @pl.when(z + 1 < sp)
    def _():
        greet({"sp": z + 1})

    @pl.when(z >= 1)
    def _():
        greet({"sp": z - 1})

    odd = lax.rem(t, 2)
    partner = place + 2 * odd - 1
    outside = jnp.logical_and(partner >= 0, partner < sp * tp)

    @pl.when(outside)
    def _():
        greet({"sp": partner // tp, "tp": lax.rem(partner, tp)})

    loads = []
    for layer in range(layers):
        for which, ref in enumerate((w_b, w_c, w_x)):
            loads.append(
                pltpu.make_async_copy(
                    ref.at[layer],
                    win.at[
                        layer,
                        which,
                        pl.ds(pl.multiple_of(z * rows, 16), rows),
                        pl.ds(pl.multiple_of(t * cols, 128), cols),
                    ],
                    load_sem.at[4 * layer + which],
                )
            )
        loads.append(
            pltpu.make_async_copy(
                w_out.at[layer],
                wout.at[
                    layer,
                    pl.ds(pl.multiple_of(t * cols, 16), cols),
                    pl.ds(pl.multiple_of(z * rows, 128), rows),
                ],
                load_sem.at[4 * layer + 3],
            )
        )
    tokens_in = pltpu.make_async_copy(
        tok, xs.at[pl.ds(halo, own_tokens)], load_sem.at[4 * layers]
    )
    for load in loads:
        load.start()
    tokens_in.start()

    after = lax.rem(place + 1, sp * tp)

    def halo_copy():
        return pltpu.make_async_remote_copy(
            src_ref=tok.at[pl.ds(own_tokens - halo, halo)],
            dst_ref=xs.at[pl.ds(0, halo)],
            send_sem=halo_sem.at[0],
            recv_sem=halo_sem.at[1],
            device_id={"sp": after // tp, "tp": lax.rem(after, tp)},
            device_id_type=MESH,
        )

    greeted = (
        3
        + jnp.where(z + 1 < sp, 1, 0)
        + jnp.where(z >= 1, 1, 0)
        + jnp.where(outside, 1, 0)
    )
    pl.semaphore_wait(ready, greeted)
    for load in loads:
        load.wait()
    own(0)

    @pl.when(place + 1 < sp * tp)
    def _():
        halo_copy().start()

    own(1)
    prod[pl.ds(0, 8), :] = jnp.zeros((8, prod.shape[1]), jnp.float32)

    @pl.when(place == 0)
    def _():
        xs[pl.ds(0, halo), :] = jnp.zeros((halo, xs.shape[1]), jnp.bfloat16)

    tokens_in.wait()

    def first_norm(start, count):
        where = pl.ds(start, count)
        hid[where, :] = scaled(xs[where, :].astype(jnp.float32), gain_pre[0][None, :]).astype(
            jnp.bfloat16
        )

    piece = own_tokens // 3
    for i in range(3):
        first_norm(halo + i * piece, piece)

    @pl.when(place > 0)
    def _():
        halo_copy().wait_recv()

    first_norm(0, halo)

    steps = sp - 1
    width = prod.shape[1]
    parts = channels // width
    work = {}

    def last_rows(layer, i):
        project_out(layer, halo + i * piece, piece)

    late_x, late_y = 2, 4
    last_step = steps * len(units) + late_y
    for u, (layer, kind) in enumerate(units):
        ready = min(steps * u + steps + late_y, last_step)
        todo = [functools.partial(arrived, u)]
        if kind == 2:
            todo += [functools.partial(project_in, layer, p, width) for p in range(parts)]
        if kind == 3:
            todo += [functools.partial(last_rows, layer, i) for i in range(3)]
            if layer + 1 < layers:
                todo.append(functools.partial(project_out, layer, 0, halo))
        for k, task in enumerate(todo):
            work.setdefault(min(ready + max(k - 1, 0), last_step), []).append(task)

    for g in range(1, last_step + 1):
        u, j = (g - 1) // steps, (g - 1) % steps + 1
        if u < len(units):
            if j == 1 and 1 <= u < len(units) - 1:
                own(u + 1)
            wave_z(u, j)
        for late, wave in ((late_x, wave_x), (late_y, wave_y)):
            v, k = (g - 1 - late) // steps, (g - 1 - late) % steps + 1
            if k == 1 and 0 <= v < len(units):
                wave(v, 0)
            if 0 <= v < len(units):
                wave(v, k)
        for task in work.get(g, []):
            task()

    for u in range(len(units)):
        sent(u)

    @pl.when(place + 1 < sp * tp)
    def _():
        halo_copy().wait_send()


def in_one_kernel(sp, tp, tokens, gain_pre, gain_post, w_b, w_c, w_x, taps, w_out):
    layers, rows, cols = w_b.shape
    own_tokens, width = tokens.shape
    channels = cols * tp
    halo = 16
    units = 4 * layers
    any_space = pl.BlockSpec(memory_space=pl.ANY)
    vmem = pl.BlockSpec(memory_space=pltpu.VMEM)
    dma = pltpu.SemaphoreType.DMA
    part = min(256, channels)
    return pl.pallas_call(
        functools.partial(mixer_kernel, sp, tp, halo),
        out_shape=pltpu.VMEM(tokens.shape, tokens.dtype),
        in_specs=[any_space, vmem, vmem, any_space, any_space, any_space, vmem, any_space],
        out_specs=vmem,
        scratch_shapes=[
            pltpu.VMEM((layers, 3, rows * sp, channels), jnp.bfloat16),
            pltpu.VMEM((layers, channels, rows * sp), jnp.bfloat16),
            pltpu.VMEM((own_tokens + halo, width), jnp.bfloat16),
            pltpu.VMEM((own_tokens + halo, width), jnp.bfloat16),
            pltpu.VMEM((own_tokens + halo, channels), jnp.bfloat16),
            pltpu.VMEM((own_tokens + halo + 8, part), jnp.float32),
            dma((4 * layers + 1,)),
            dma((2,)),
            dma((units, sp, 2)),
            dma((units, sp)),
            dma((units, sp)),
            dma((units, sp)),
            dma((units, sp)),
            dma((units, sp)),
            dma((units, sp)),
            dma((units, sp)),
            dma((units, sp, 2)),
            dma((units, sp, 2)),
        ],
        compiler_params=pltpu.CompilerParams(
            has_side_effects=True, collective_id=0, vmem_limit_bytes=56000 * 1024
        ),
    )(tokens, gain_pre, gain_post, w_b, w_c, w_x, jnp.swapaxes(taps, 0, 1), w_out)


def kernel_fits(sizes, tokens, w_b, w_out, taps):
    rows, cols = w_b.shape[1], w_b.shape[2]
    layers = w_b.shape[0]
    held = (4 * layers * rows * sizes["sp"] * cols * sizes["tp"]) * 2
    held += 3 * tokens.shape[0] * tokens.shape[1] * 2
    return (
        sizes["grp"] == 2
        and sizes["tp"] == 4
        and rows % 128 == 0
        and cols % 128 == 0
        and tokens.shape[0] % 48 == 0
        and (taps.shape[1] - 1) * layers <= 16
        and taps.shape[1] <= 9
        and held < 40 * 2**20
    )


def any_mesh(sizes, *arguments):
    tokens, w_b, taps, w_out = arguments[0], arguments[3], arguments[6], arguments[7]
    if kernel_fits(sizes, tokens, w_b, w_out, taps):
        return in_one_kernel(sizes["sp"], sizes["tp"], *arguments)
    return on_device(*arguments)


def solution(mesh):
    placed = (
        P(("grp", "sp", "tp"), None),
        P(),
        P(),
        P(None, "sp", "tp"),
        P(None, "sp", "tp"),
        P(None, "sp", "tp"),
        P(),
        P(None, "tp", "sp"),
    )
    return jax.shard_map(
        functools.partial(any_mesh, dict(mesh.shape)),
        mesh=mesh,
        in_specs=placed,
        out_specs=P(("grp", "sp", "tp"), None),
        check_vma=False,
    )
```
